32 devices in a mesh: kv: 8 (over z, x), tp: 4 (over y, core).
Axes of the slice: x: 2, y: 2, z: 4, core: 2. Of those that a mesh axis runs over, the one named last changes fastest.
Arguments:
- inputs: bfloat16 [2048, 2048], P('kv', 'tp'), may hold values from -6 to 6
- queries: bfloat16 [2048, 2048], P('kv', 'tp'), may hold values from -8 to 8
- key_vectors: bfloat16 [2048, 512], P('kv', 'tp'), may hold values from -8 to 8
- value_rows_by_head: bfloat16 [2048, 512], P('kv', 'tp'), may hold values from -6 to 6
- out_grad: bfloat16 [2048, 2048], P('kv', 'tp'), may hold values from -6 to 6
- chosen: int32 [16, 16], replicated, may hold values from 0 to 31, as said below
Outputs:
- query_grad: bfloat16 [2048, 2048], P('kv', 'tp')
- key_grad: bfloat16 [2048, 512], P('kv', 'tp')
- value_grad: bfloat16 [2048, 512], P('kv', 'tp')
- weight_grad: float32 [2048, 2048], P('kv', 'tp')
The draws below stay inside these ranges and needn't reach their ends.
Inputs may be any that keep to these rules, and one draw needn't show every extreme that they name: `chosen`: row r holds 16 distinct key-block numbers, among them every key block that intersects query block r. The rows of one device (aligned runs of 2 rows) name at most 2 distinct key blocks that lie on any one other device (aligned runs of 4 key blocks), and exactly 2 at some other device for some devices.
All inputs are finite; a program needn't handle non-finite values.
Results may differ from the reference program's by a relative error of at most 0.015.
The reference program's roundings to bfloat16 on the way (of `probs_half` and `score_grad`) count: a program that leaves them out, or rounds other values in their place, can miss the bound.
Values may be sent and summed in bfloat16 or wider, within the bound.
A program may use at most 128 MiB of HBM per device.

```python
import jax
import jax.numpy as jnp
from jax import lax

D = 2048
QUERY_HEADS = 32
KEY_VALUE_HEADS = 8
HEAD_SIZE = 64
QB = 128
KB = 64
NSEL = 16
TOK_DEV = 256
SEQUENCE_TOKENS = 2048


def draw_queries(key, part):
    final_result = jnp.clip(jax.random.normal(jax.random.fold_in(key, 1), (SEQUENCE_TOKENS, QUERY_HEADS * HEAD_SIZE), jnp.float32), -6.0, 6.0)
    return final_result.astype(jnp.bfloat16)


def draw_key_vectors(key, part):
    final_result = jnp.clip(jax.random.normal(jax.random.fold_in(key, 2), (SEQUENCE_TOKENS, KEY_VALUE_HEADS * HEAD_SIZE), jnp.float32), -6.0, 6.0)
    return final_result.astype(jnp.bfloat16)


def draw_chosen(key, part):
    q_count = SEQUENCE_TOKENS // QB
    k_count = SEQUENCE_TOKENS // KB
    ratio = QB // KB
    owner_blocks = TOK_DEV // KB
    local_blocks = TOK_DEV // QB
    n_dev = SEQUENCE_TOKENS // TOK_DEV
    q_index = jnp.arange(q_count, dtype=jnp.int32)[:, None]
    k_index = jnp.arange(k_count, dtype=jnp.int32)[None, :]
    dev_grid = jnp.arange(n_dev, dtype=jnp.int32)[:, None]
    own_grid = jnp.arange(n_dev, dtype=jnp.int32)[None, :]
    random_phase = jax.random.randint(jax.random.fold_in(key, 7), (n_dev, n_dev), 0, ratio)
    phase = jnp.where(own_grid == (dev_grid - 1) % n_dev, ratio - 1, jnp.where(own_grid == (dev_grid - n_dev // 2) % n_dev, 0, random_phase))
    query_dev = q_index // local_blocks
    key_owner = k_index // owner_blocks
    key_offset = k_index % owner_blocks
    permitted = (key_owner == query_dev) | (key_offset % ratio == phase[query_dev, key_owner])
    own_block = k_index // ratio == q_index
    forced = (k_index == q_index * ratio - 1) | (k_index == q_index * ratio - k_count // 2)
    causal = k_index < q_index * ratio
    tier = jnp.where(own_block, 3, jnp.where(forced, 2, jnp.where(causal, 1, 0)))
    tier = jnp.where(permitted, tier, -1)
    popular = jax.random.randint(jax.random.fold_in(key, 5), (k_count,), 0, 2) * 7
    row_keys = jax.random.split(jax.random.fold_in(key, 6), q_count)
    noise = jax.vmap(lambda one_key: jax.random.permutation(one_key, k_count))(row_keys)
    ranking = tier * (k_count * 8) + popular[None, :] * k_count + noise
    _, picked = lax.top_k(ranking, NSEL)
    return picked.astype(jnp.int32)


def levels(rng, dims, shards, least, largest):
    loudness = 1.0
    for dim, parts in shards:
        draws = jax.random.uniform(jax.random.fold_in(jax.random.fold_in(rng, 6), dim), (parts,), jnp.float32, least / len(shards), largest / len(shards))
        loudness = loudness * jnp.repeat(jnp.exp(draws), dims[dim] // parts).reshape((-1,) + (1,) * (len(dims) - 1 - dim))
    return loudness


def centred(stream_key, dims, deviation, limit, shards=(), kind=jnp.bfloat16):
    level = levels(stream_key, dims, shards, -0.22, 0.18) if shards else 1.0
    entries = jax.random.normal(stream_key, dims, jnp.float32) * deviation * level
    return jnp.minimum(jnp.maximum(entries, -limit), limit).astype(kind)


def setup_inputs(seed: int = 0) -> dict:
    streams_of = jax.random.split(jax.random.key(seed), 7)
    inputs = centred(streams_of[0], (SEQUENCE_TOKENS, D), 1.0, 6.0, ((0, 8), (1, 4)))
    queries = draw_queries(jax.random.fold_in(streams_of[6], 71), 0)
    key_vectors = draw_key_vectors(jax.random.fold_in(streams_of[6], 71), 0)
    value_rows_by_head = centred(streams_of[3], (SEQUENCE_TOKENS, KEY_VALUE_HEADS * HEAD_SIZE), 1.0, 6.0, ((0, 8), (1, 4)))
    out_grad = centred(streams_of[4], (SEQUENCE_TOKENS, QUERY_HEADS * HEAD_SIZE), 1.0, 6.0, ((0, 8), (1, 4)))
    chosen = draw_chosen(jax.random.fold_in(streams_of[6], 71), 0)
    return dict(inputs=inputs, queries=queries, key_vectors=key_vectors, value_rows_by_head=value_rows_by_head, out_grad=out_grad, chosen=chosen)


def round_trip(values_in):
    halved = lax.optimization_barrier(values_in.astype(jnp.bfloat16))
    return halved.astype(jnp.float32)


def reference(inputs, queries, key_vectors, value_rows_by_head, out_grad, chosen):
    total = queries.shape[0]
    q_heads = queries.shape[1] // HEAD_SIZE
    kv_heads = key_vectors.shape[1] // HEAD_SIZE
    group_size = q_heads // kv_heads
    score_scale = HEAD_SIZE ** -0.5
    offsets = jnp.arange(KB, dtype=jnp.int32)

    def step(state_pair, q_blk):
        acc_k, acc_v = state_pair
        first = q_blk * QB
        q_block = lax.dynamic_slice_in_dim(queries, first, QB, 0).astype(jnp.float32).reshape(QB, kv_heads, group_size, HEAD_SIZE)
        g_block = lax.dynamic_slice_in_dim(out_grad, first, QB, 0).astype(jnp.float32).reshape(QB, kv_heads, group_size, HEAD_SIZE)
        key_rows = (chosen[q_blk][:, None] * KB + offsets[None, :]).reshape(-1).astype(jnp.int32)
        key_sel = key_vectors[key_rows].astype(jnp.float32).reshape(-1, kv_heads, HEAD_SIZE)
        val_sel = value_rows_by_head[key_rows].astype(jnp.float32).reshape(-1, kv_heads, HEAD_SIZE)
        positions = first + jnp.arange(QB, dtype=jnp.int32)
        allowed = key_rows[None, :] <= positions[:, None]
        scores = jnp.einsum('tkgd,skd->kgts', q_block, key_sel) * score_scale
        scores = jnp.where(allowed, scores, -1e30)
        row_max = jnp.max(scores, axis=-1, keepdims=True)
        log_sum = row_max + jnp.log(jnp.sum(jnp.exp(scores - row_max), axis=-1, keepdims=True))
        probs = jnp.exp(scores - log_sum)
        probs_half = round_trip(probs)
        attended = jnp.einsum('kgts,skd->tkgd', probs_half, val_sel)
        row_dot = jnp.einsum('tkgd,tkgd->kgt', g_block, attended)
        prob_grad = jnp.einsum('tkgd,skd->kgts', g_block, val_sel)
        score_grad = round_trip(probs * (prob_grad - row_dot[..., None]))
        d_query = jnp.einsum('kgts,skd->tkgd', score_grad, key_sel) * score_scale
        d_key = jnp.einsum('kgts,tkgd->skd', score_grad, q_block) * score_scale
        d_value = jnp.einsum('kgts,tkgd->skd', probs_half, g_block)
        acc_k = acc_k.at[key_rows].add(d_key.reshape(-1, kv_heads * HEAD_SIZE))
        acc_v = acc_v.at[key_rows].add(d_value.reshape(-1, kv_heads * HEAD_SIZE))
        return (acc_k, acc_v), d_query.reshape(QB, q_heads * HEAD_SIZE)

    zeros = jnp.zeros((total, kv_heads * HEAD_SIZE), jnp.float32)
    (acc_k, acc_v), query_blocks = lax.scan(step, (zeros, zeros), jnp.arange(total // QB, dtype=jnp.int32))
    query_grad = query_blocks.reshape(total, q_heads * HEAD_SIZE).astype(jnp.bfloat16)
    weight_grad = jnp.dot(inputs.T, query_grad, preferred_element_type=jnp.float32)
    return query_grad, acc_k.astype(jnp.bfloat16), acc_v.astype(jnp.bfloat16), weight_grad
```

```python
import functools

import jax
import jax.numpy as jnp
from jax import lax
from jax.experimental import pallas as pl
from jax.experimental.pallas import tpu as pltpu
from jax.sharding import PartitionSpec as P

HEAD_SIZE = 64
QB = 128
KB = 64
HEADS_PER_KEY = 4
NEG = -1e30
BF16 = jnp.bfloat16
F32 = jnp.float32


def dot_nt(x, y):
    return lax.dot_general(x, y, (((1,), (1,)), ((), ())), preferred_element_type=F32)


def dot_nn(x, y):
    return lax.dot_general(x, y, (((1,), (0,)), ((), ())), preferred_element_type=F32)


def dot_tn(x, y):
    return lax.dot_general(x, y, (((0,), (0,)), ((), ())), preferred_element_type=F32)


def kernel(
    n, tp, a, b,
    sel_ref, x_ref, q_ref, k_ref, v_ref, g_ref,
    dq_ref, dk_ref, dv_ref, w_ref,
    kvst, kvbuf, xst, xbuf, q_s, g_s, s_buf, dp_buf, dq_acc, gst, grecv, own_acc,
    qall, wst, wrecv, w_own,
    kv_send, kv_recv, x_send, x_recv, g_send, g_recv, q_send, q_recv, w_send, w_recv,
):
    me = lax.axis_index("kv")
    t = lax.axis_index("tp")
    alpha = lax.rem(me, a)
    beta = lax.div(me, a)
    rows, cols = k_ref.shape
    heads = cols // HEAD_SIZE
    group = q_ref.shape[1] // cols
    local = rows // QB
    owner = rows // KB
    chunk = local * KB
    own_chunks = rows // chunk
    wide = group * rows
    width = xst.shape[2]
    n_chunk = xst.shape[0]
    gcols = group * HEAD_SIZE
    scale = HEAD_SIZE ** (-0.5)

    def remote(src, dst, send, recv, kv, tpi):
        return pltpu.make_async_remote_copy(
            src_ref=src, dst_ref=dst, send_sem=send, recv_sem=recv,
            device_id=(kv, tpi), device_id_type=pl.DeviceIdType.MESH,
        )

    barrier = pltpu.get_barrier_semaphore()
    for d in range(1, n):
        pl.semaphore_signal(
            barrier, inc=1, device_id=(lax.rem(me + d, n), t), device_id_type=pl.DeviceIdType.MESH
        )
    for d in range(1, tp):
        for m in range(a):
            pl.semaphore_signal(
                barrier, inc=1, device_id=(beta * a + m, lax.rem(t + d, tp)),
                device_id_type=pl.DeviceIdType.MESH,
            )

    def slots(i, j):
        used = []
        for blk in range(owner):
            u = sel_ref[i * local, j * owner + blk]
            for r in range(1, local):
                u = jnp.maximum(u, sel_ref[i * local + r, j * owner + blk])
            used.append(u)
        picks = []
        for p in range(local):
            before = jnp.int32(0)
            one = []
            for blk in range(owner):
                one.append(jnp.where(before == p, used[blk], 0))
                before = before + used[blk]
            picks.append(one)
        return picks

    def stage_kv(i, carry):
        picks = slots(i, me)
        for p in range(local):
            at = slice(p * KB, (p + 1) * KB)
            for ref, first in ((k_ref, 0), (v_ref, cols)):
                out = jnp.zeros((KB, cols), F32)
                for blk in range(owner):
                    rows_of = ref[blk * KB : (blk + 1) * KB, :].astype(F32)
                    out = jnp.where(picks[p][blk] > 0, rows_of, out)
                kvst[i, at, first : first + cols] = out.astype(BF16)
        return carry

    lax.fori_loop(me + 1, n, stage_kv, 0)
    for q in range(n_chunk):
        xst[q] = x_ref[:, q * width : (q + 1) * width]

    pl.semaphore_wait(barrier, n - 1 + (tp - 1) * a)

    def kv_copy(i, j):
        return remote(kvst.at[i], kvbuf.at[j], kv_send.at[i], kv_recv.at[j], i, t)

    def start_kv(i, carry):
        kv_copy(i, me).start()
        return carry

    lax.fori_loop(me + 1, n, start_kv, 0)

    def x_copy(q, tt):
        c = t * n_chunk + q
        return remote(
            xst.at[q], xbuf.at[alpha, lax.div(c, a)], x_send.at[q, tt],
            x_recv.at[alpha, lax.div(c, a)], beta * a + lax.rem(c, a), tt,
        )

    for q in range(n_chunk):
        c = t * n_chunk + q
        for tt in range(tp):
            mine = jnp.logical_and(lax.rem(c, a) == alpha, t == tt)

            @pl.when(jnp.logical_not(mine))
            def _():
                x_copy(q, tt).start()

            @pl.when(mine)
            def _():
                xbuf[alpha, lax.div(c, a)] = x_ref[:, q * width : (q + 1) * width]

    lane = lax.rem(lax.broadcasted_iota(jnp.int32, (1, wide), 1), rows)
    lane_block = lax.div(lane, QB)

    def row_bias(flags):
        vals = [jnp.where(f > 0, F32(0.0), F32(NEG)) for f in flags]
        out = jnp.full((1, wide), vals[0], F32)
        for r in range(1, local):
            out = jnp.where(lane_block == r, vals[r], out)
        return out

    def head_cols(h):
        return slice(h * HEAD_SIZE, (h + 1) * HEAD_SIZE)

    def own_kv(o, h):
        at = slice(o * chunk, (o + 1) * chunk)
        return k_ref[at, head_cols(h)], v_ref[at, head_cols(h)]

    def far_k(j, h):
        return kvbuf[j, :, head_cols(h)]

    def far_v(j, h):
        return kvbuf[j, :, cols + h * HEAD_SIZE : cols + (h + 1) * HEAD_SIZE]

    def g_copy(h, i, j):
        return remote(gst.at[h, j], grecv.at[h, i], g_send.at[h, j], g_recv.at[h, i], j, t)

    def q_copy(h, m):
        return remote(
            qall.at[h, alpha], qall.at[h, alpha], q_send.at[h, m], q_recv.at[h, alpha],
            beta * a + m, t,
        )

    def w_copy(h, bb):
        return remote(
            wst.at[h, bb], wrecv.at[h, beta], w_send.at[h, bb], w_recv.at[h, beta],
            bb * a + alpha, t,
        )

    def score_own(o, h):
        k, _ = own_kv(o, h)
        s = dot_nt(k, q_s[...])
        parts = []
        for p in range(local):
            blk = o * local + p
            bias = row_bias([sel_ref[me * local + r, me * owner + blk] for r in range(local)])
            key = blk * KB + lax.broadcasted_iota(jnp.int32, (KB, wide), 0)
            parts.append(jnp.where(key <= lane, s[p * KB : (p + 1) * KB] + bias, NEG))
        return jnp.concatenate(parts, axis=0)

    def attend(h, wait_kv):
        for gr in range(group):
            hh = h * group + gr
            at = slice(gr * rows, (gr + 1) * rows)
            q_s[at, :] = (q_ref[:, head_cols(hh)].astype(F32) * scale).astype(BF16)
            g_s[at, :] = g_ref[:, head_cols(hh)]
        m = jnp.full((1, wide), NEG, F32)
        for o in range(own_chunks):
            s = score_own(o, h)
            s_buf[o] = s
            m = jnp.maximum(m, jnp.max(s, axis=0, keepdims=True))

        def pass_a(j, m):
            if wait_kv:
                kv_copy(j, j).wait_recv()
            picks = slots(me, j)
            s = dot_nt(far_k(j, h), q_s[...])
            parts = []
            for p in range(local):
                flags = []
                for r in range(local):
                    f = jnp.int32(0)
                    for blk in range(owner):
                        f = f + picks[p][blk] * sel_ref[me * local + r, j * owner + blk]
                    flags.append(f)
                parts.append(s[p * KB : (p + 1) * KB] + row_bias(flags))
            s = jnp.concatenate(parts, axis=0)
            s_buf[own_chunks + j] = s
            return jnp.maximum(m, jnp.max(s, axis=0, keepdims=True))

        m = lax.fori_loop(0, me, pass_a, m)

        def pass_b(idx, v, l, rd):
            p = jnp.exp(s_buf[idx] - m)
            dp = dot_nt(v, g_s[...])
            s_buf[idx] = p
            dp_buf[idx] = dp
            return (
                l + jnp.sum(p, axis=0, keepdims=True),
                rd + jnp.sum(p * dp, axis=0, keepdims=True),
            )

        l = jnp.zeros((1, wide), F32)
        rd = jnp.zeros((1, wide), F32)
        for o in range(own_chunks):
            l, rd = pass_b(o, own_kv(o, h)[1], l, rd)
        l, rd = lax.fori_loop(
            0, me, lambda j, c: pass_b(own_chunks + j, far_v(j, h), c[0], c[1]), (l, rd)
        )
        inv = 1.0 / l
        rd = rd * inv

        def pass_c(idx, k):
            pn = s_buf[idx] * inv
            ds = (pn * (dp_buf[idx] - rd)).astype(BF16)
            dv = dot_nn(pn.astype(BF16), g_s[...])
            dk = dot_nn(ds, q_s[...])
            return dot_tn(ds, k), dk, dv

        def far_c(j, carry):
            dq, dk, dv = pass_c(own_chunks + j, far_k(j, h))
            gst[h, j, :, 0:HEAD_SIZE] = dk.astype(BF16)
            gst[h, j, :, HEAD_SIZE : 2 * HEAD_SIZE] = dv.astype(BF16)
            dq_acc[...] += dq
            g_copy(h, me, j).start()
            return carry

        for o in range(own_chunks):
            dq, dk, dv = pass_c(o, own_kv(o, h)[0])
            at = slice(o * chunk, (o + 1) * chunk)
            own_acc[h, at, 0:HEAD_SIZE] = dk
            own_acc[h, at, HEAD_SIZE : 2 * HEAD_SIZE] = dv
            if o == 0:
                dq_acc[...] = dq
            else:
                dq_acc[...] += dq
        lax.fori_loop(0, me, far_c, 0)
        for gr in range(group):
            part = (dq_acc[gr * rows : (gr + 1) * rows, :] * scale).astype(BF16)
            dq_ref[:, head_cols(h * group + gr)] = part
            qall[h, alpha, :, head_cols(gr)] = part
        for mm in range(a):

            @pl.when(alpha != mm)
            def _():
                q_copy(h, mm).start()

    def weight_part(h, wait_x):
        if wait_x:
            for m in range(a):
                for bb in range(b):
                    own = jnp.logical_and(alpha == m, lax.div(bb * a + alpha, n_chunk) == t)

                    @pl.when(jnp.logical_not(own))
                    def _():
                        remote(
                            xst.at[0], xbuf.at[m, bb], x_send.at[0, 0], x_recv.at[m, bb], me, t
                        ).wait_recv()

        for mm in range(a):

            @pl.when(alpha != mm)
            def _():
                remote(
                    qall.at[h, mm], qall.at[h, mm], q_send.at[h, mm], q_recv.at[h, mm], me, t
                ).wait_recv()

        def partial(bb):
            out = dot_tn(xbuf[0, bb], qall[h, 0])
            for m in range(1, a):
                out = out + dot_tn(xbuf[m, bb], qall[h, m])
            return out

        for d in range(1, b):
            bb = lax.rem(beta + d, b)
            wst[h, bb] = partial(bb).astype(BF16)
            w_copy(h, bb).start()
        w_own[h] = partial(beta)

    for h in range(heads):
        attend(h, h == 0)
    for h in range(heads):
        weight_part(h, h == 0)

    for h in range(heads):

        def add_far(i, carry):
            remote(gst.at[h, 0], grecv.at[h, i], g_send.at[h, 0], g_recv.at[h, i], me, t).wait_recv()
            picks = slots(i, me)
            for p in range(local):
                got = grecv[h, i, p * KB : (p + 1) * KB, :].astype(F32)
                for blk in range(owner):
                    own_acc[h, blk * KB : (blk + 1) * KB, :] += jnp.where(
                        picks[p][blk] > 0, got, 0.0
                    )
            return carry

        lax.fori_loop(me + 1, n, add_far, 0)
        dk_ref[:, head_cols(h)] = own_acc[h, :, 0:HEAD_SIZE].astype(BF16)
        dv_ref[:, head_cols(h)] = own_acc[h, :, HEAD_SIZE : 2 * HEAD_SIZE].astype(BF16)

    for h in range(heads):
        total = w_own[h]
        for d in range(1, b):
            bb = lax.rem(beta + d, b)
            remote(
                wst.at[h, bb], wrecv.at[h, bb], w_send.at[h, bb], w_recv.at[h, bb], me, t
            ).wait_recv()
            total = total + wrecv[h, bb].astype(F32)
        w_ref[:, h * gcols : (h + 1) * gcols] = total

    def done_kv(i, carry):
        kv_copy(i, me).wait_send()
        return carry

    lax.fori_loop(me + 1, n, done_kv, 0)
    for q in range(n_chunk):
        c = t * n_chunk + q
        for tt in range(tp):

            @pl.when(jnp.logical_not(jnp.logical_and(lax.rem(c, a) == alpha, t == tt)))
            def _():
                x_copy(q, tt).wait_send()

    for h in range(heads):

        def done_g(j, carry):
            g_copy(h, me, j).wait_send()
            return carry

        lax.fori_loop(0, me, done_g, 0)
        for mm in range(a):

            @pl.when(alpha != mm)
            def _():
                q_copy(h, mm).wait_send()

        for d in range(1, b):
            w_copy(h, lax.rem(beta + d, b)).wait_send()


def body(n, tp, inputs, queries, key_vectors, value_rows_by_head, out_grad, chosen):
    rows, cols = key_vectors.shape
    q_cols = queries.shape[1]
    heads = cols // HEAD_SIZE
    group = q_cols // cols
    local = rows // QB
    chunk = local * KB
    own_chunks = rows // chunk
    wide = group * rows
    d_model = inputs.shape[1] * tp
    width = d_model // n
    n_chunk = inputs.shape[1] // width
    a = 4
    b = n // a
    gcols = group * HEAD_SIZE
    blocks = n * rows // KB
    sel = jnp.any(
        chosen[:, :, None] == jnp.arange(blocks, dtype=jnp.int32)[None, None, :], axis=1
    ).astype(jnp.int32)
    vmem = pl.BlockSpec(memory_space=pltpu.VMEM)
    dma = pltpu.SemaphoreType.DMA
    return pl.pallas_call(
        functools.partial(kernel, n, tp, a, b),
        out_shape=(
            jax.ShapeDtypeStruct((rows, q_cols), BF16),
            jax.ShapeDtypeStruct((rows, cols), BF16),
            jax.ShapeDtypeStruct((rows, cols), BF16),
            jax.ShapeDtypeStruct((width, q_cols), F32),
        ),
        in_specs=[pl.BlockSpec(memory_space=pltpu.SMEM)] + [vmem] * 5,
        out_specs=(vmem,) * 4,
        scratch_shapes=[
            pltpu.VMEM((n, chunk, 2 * cols), BF16),
            pltpu.VMEM((n, chunk, 2 * cols), BF16),
            pltpu.VMEM((n_chunk, rows, width), BF16),
            pltpu.VMEM((a, b, rows, width), BF16),
            pltpu.VMEM((wide, HEAD_SIZE), BF16),
            pltpu.VMEM((wide, HEAD_SIZE), BF16),
            pltpu.VMEM((own_chunks + n - 1, chunk, wide), F32),
            pltpu.VMEM((own_chunks + n - 1, chunk, wide), F32),
            pltpu.VMEM((wide, HEAD_SIZE), F32),
            pltpu.VMEM((heads, n, chunk, 2 * HEAD_SIZE), BF16),
            pltpu.VMEM((heads, n, chunk, 2 * HEAD_SIZE), BF16),
            pltpu.VMEM((heads, rows, 2 * HEAD_SIZE), F32),
            pltpu.VMEM((heads, a, rows, gcols), BF16),
            pltpu.VMEM((heads, b, width, gcols), BF16),
            pltpu.VMEM((heads, b, width, gcols), BF16),
            pltpu.VMEM((heads, width, gcols), F32),
            dma((n,)),
            dma((n,)),
            dma((n_chunk, tp)),
            dma((a, b)),
            dma((heads, n)),
            dma((heads, n)),
            dma((heads, a)),
            dma((heads, a)),
            dma((heads, b)),
            dma((heads, b)),
        ],
        compiler_params=pltpu.CompilerParams(
            collective_id=0, has_side_effects=True, vmem_limit_bytes=60 * 1024 * 1024
        ),
    )(sel, inputs, queries, key_vectors, value_rows_by_head, out_grad)


def solution(mesh):
    n, tp = mesh.shape["kv"], mesh.shape["tp"]
    placed = (P("kv", "tp"),) * 5 + (P(),)
    return jax.shard_map(
        functools.partial(body, n, tp),
        mesh=mesh,
        in_specs=placed,
        out_specs=(P("kv", "tp"),) * 4,
        check_vma=False,
    )
```

```python
import functools

import jax
import jax.numpy as jnp
from jax import lax
from jax.experimental import pallas as pl
from jax.experimental.pallas import tpu as pltpu
from jax.sharding import PartitionSpec as P

HEAD_SIZE = 64
QB = 128
KB = 64
PARTS = 2
HEADS_PER_KEY = 4
NEG = -1e30
BF16 = jnp.bfloat16
F32 = jnp.float32


def dot_nt(x, y):
    return lax.dot_general(x, y, (((1,), (1,)), ((), ())), preferred_element_type=F32)


def dot_nn(x, y):
    return lax.dot_general(x, y, (((1,), (0,)), ((), ())), preferred_element_type=F32)


def dot_tn(x, y):
    return lax.dot_general(x, y, (((0,), (0,)), ((), ())), preferred_element_type=F32)


def kernel(
    n, tp, a, b,
    sel_ref, x_ref, q_ref, k_ref, v_ref, g_ref,
    dq_ref, dk_ref, dv_ref, w_ref,
    kvst, kvbuf, xst, xbuf, q_s, g_s, s_buf, dp_buf, dq_acc, far_acc, gst, grecv, own_acc,
    qall, wst, wrecv, w_own,
    kv_send, kv_recv, x_send, xf_send, x_recv, g_send, g_recv, q_send, q_recv, w_send, w_recv,
):
    me = lax.axis_index("kv")
    t = lax.axis_index("tp")
    alpha = lax.rem(me, a)
    beta = lax.div(me, a)
    rows, cols = k_ref.shape
    heads = cols // HEAD_SIZE
    group = q_ref.shape[1] // cols
    local = rows // QB
    owner = rows // KB
    chunk = local * KB
    own_chunks = rows // chunk
    sub = group // PARTS
    wide = sub * rows
    width = xst.shape[2]
    n_chunk = xst.shape[0]
    gcols = sub * HEAD_SIZE
    scale = HEAD_SIZE ** (-0.5)

    def remote(src, dst, send, recv, kv, tpi):
        return pltpu.make_async_remote_copy(
            src_ref=src, dst_ref=dst, send_sem=send, recv_sem=recv,
            device_id=(kv, tpi), device_id_type=pl.DeviceIdType.MESH,
        )

    barrier = pltpu.get_barrier_semaphore()
    for d in range(1, n):
        pl.semaphore_signal(
            barrier, inc=1, device_id=(lax.rem(me + d, n), t), device_id_type=pl.DeviceIdType.MESH
        )
    for d in range(1, tp):
        for m in range(a):
            pl.semaphore_signal(
                barrier, inc=1, device_id=(beta * a + m, lax.rem(t + d, tp)),
                device_id_type=pl.DeviceIdType.MESH,
            )

    def slots(i, j):
        used = []
        for blk in range(owner):
            u = sel_ref[i * local, j * owner + blk]
            for r in range(1, local):
                u = jnp.maximum(u, sel_ref[i * local + r, j * owner + blk])
            used.append(u)
        picks = []
        for p in range(local):
            before = jnp.int32(0)
            one = []
            for blk in range(owner):
                one.append(jnp.where(before == p, used[blk], 0))
                before = before + used[blk]
            picks.append(one)
        return picks

    def stage_kv(i, carry):
        picks = slots(i, me)
        for p in range(local):
            at = slice(p * KB, (p + 1) * KB)
            for ref, first in ((k_ref, 0), (v_ref, cols)):
                out = jnp.zeros((KB, cols), F32)
                for blk in range(owner):
                    rows_of = ref[blk * KB : (blk + 1) * KB, :].astype(F32)
                    out = jnp.where(picks[p][blk] > 0, rows_of, out)
                kvst[i, at, first : first + cols] = out.astype(BF16)
        return carry

    lax.fori_loop(me + 1, n, stage_kv, 0)
    for q in range(n_chunk):
        xst[q] = x_ref[:, q * width : (q + 1) * width]

    pl.semaphore_wait(barrier, n - 1 + (tp - 1) * a)

    def kv_copy(i, j):
        return remote(kvst.at[i], kvbuf.at[j], kv_send.at[i], kv_recv.at[j], i, t)

    def start_kv(i, carry):
        kv_copy(i, me).start()
        return carry

    lax.fori_loop(me + 1, n, start_kv, 0)

    def x_copy(q):
        c = t * n_chunk + q
        return remote(
            xst.at[q], xbuf.at[alpha, lax.div(c, a)], x_send.at[q],
            x_recv.at[alpha, lax.div(c, a)], beta * a + lax.rem(c, a), t,
        )

    for q in range(n_chunk):
        c = t * n_chunk + q
        mine = lax.rem(c, a) == alpha

        @pl.when(jnp.logical_not(mine))
        def _():
            x_copy(q).start()

        @pl.when(mine)
        def _():
            xbuf[alpha, lax.div(c, a)] = x_ref[:, q * width : (q + 1) * width]

    def x_hand(q, m, d):
        slot = xbuf.at[m, lax.div(t * n_chunk + q, a)]
        return remote(
            slot, slot, xf_send.at[q, m, d - 1], x_recv.at[m, lax.div(t * n_chunk + q, a)],
            me, lax.rem(t + d, tp),
        )

    def forward_x():
        for q in range(n_chunk):

            @pl.when(lax.rem(t * n_chunk + q, a) == alpha)
            def _():
                for m in range(a):

                    @pl.when(alpha != m)
                    def _():
                        x_hand(q, m, 1).wait_recv()

                    for d in range(1, tp):
                        x_hand(q, m, d).start()

    lane = lax.rem(lax.broadcasted_iota(jnp.int32, (1, wide), 1), rows)
    lane_block = lax.div(lane, QB)

    def row_bias(flags):
        vals = [jnp.where(f > 0, F32(0.0), F32(NEG)) for f in flags]
        out = jnp.full((1, wide), vals[0], F32)
        for r in range(1, local):
            out = jnp.where(lane_block == r, vals[r], out)
        return out

    def head_cols(h):
        return slice(h * HEAD_SIZE, (h + 1) * HEAD_SIZE)

    def own_kv(o, h):
        at = slice(o * chunk, (o + 1) * chunk)
        return k_ref[at, head_cols(h)], v_ref[at, head_cols(h)]

    def far_k(j, h):
        return kvbuf[j, :, head_cols(h)]

    def far_v(j, h):
        return kvbuf[j, :, cols + h * HEAD_SIZE : cols + (h + 1) * HEAD_SIZE]

    def g_copy(h, i, j):
        return remote(gst.at[h, j], grecv.at[h, i], g_send.at[h, j], g_recv.at[h, i], j, t)

    def q_copy(h, m):
        return remote(
            qall.at[h, alpha], qall.at[h, alpha], q_send.at[h, m], q_recv.at[h, alpha],
            beta * a + m, t,
        )

    def w_copy(h, bb):
        return remote(
            wst.at[h, bb], wrecv.at[h, beta], w_send.at[h, bb], w_recv.at[h, beta],
            bb * a + alpha, t,
        )

    def score_own(o, h):
        k, _ = own_kv(o, h)
        s = dot_nt(k, q_s[...])
        parts = []
        for p in range(local):
            blk = o * local + p
            bias = row_bias([sel_ref[me * local + r, me * owner + blk] for r in range(local)])
            key = blk * KB + lax.broadcasted_iota(jnp.int32, (KB, wide), 0)
            parts.append(jnp.where(key <= lane, s[p * KB : (p + 1) * KB] + bias, NEG))
        return jnp.concatenate(parts, axis=0)

    def attend(u, wait_kv):
        h, part = u // PARTS, u % PARTS
        for gr in range(sub):
            hh = u * sub + gr
            at = slice(gr * rows, (gr + 1) * rows)
            q_s[at, :] = (q_ref[:, head_cols(hh)].astype(F32) * scale).astype(BF16)
            g_s[at, :] = g_ref[:, head_cols(hh)]
        m = jnp.full((1, wide), NEG, F32)
        for o in range(own_chunks):
            s = score_own(o, h)
            s_buf[o] = s
            m = jnp.maximum(m, jnp.max(s, axis=0, keepdims=True))

        def pass_a(j, m):
            if wait_kv:
                kv_copy(j, j).wait_recv()
            picks = slots(me, j)
            s = dot_nt(far_k(j, h), q_s[...])
            parts = []
            for p in range(local):
                flags = []
                for r in range(local):
                    f = jnp.int32(0)
                    for blk in range(owner):
                        f = f + picks[p][blk] * sel_ref[me * local + r, j * owner + blk]
                    flags.append(f)
                parts.append(s[p * KB : (p + 1) * KB] + row_bias(flags))
            s = jnp.concatenate(parts, axis=0)
            s_buf[own_chunks + j] = s
            return jnp.maximum(m, jnp.max(s, axis=0, keepdims=True))

        m = lax.fori_loop(0, me, pass_a, m)
        if wait_kv:
            forward_x()

        def pass_b(idx, v, l, rd):
            p = jnp.exp(s_buf[idx] - m)
            dp = dot_nt(v, g_s[...])
            s_buf[idx] = p
            dp_buf[idx] = dp
            return (
                l + jnp.sum(p, axis=0, keepdims=True),
                rd + jnp.sum(p * dp, axis=0, keepdims=True),
            )

        l = jnp.zeros((1, wide), F32)
        rd = jnp.zeros((1, wide), F32)
        for o in range(own_chunks):
            l, rd = pass_b(o, own_kv(o, h)[1], l, rd)
        l, rd = lax.fori_loop(
            0, me, lambda j, c: pass_b(own_chunks + j, far_v(j, h), c[0], c[1]), (l, rd)
        )
        if u > 0:
            weight_part(u - 1, u == 1)
        inv = 1.0 / l
        rd = rd * inv

        def pass_c(idx, k):
            pn = s_buf[idx] * inv
            ds = (pn * (dp_buf[idx] - rd)).astype(BF16)
            dv = dot_nn(pn.astype(BF16), g_s[...])
            dk = dot_nn(ds, q_s[...])
            return dot_tn(ds, k), dk, dv

        def far_c(j, carry):
            dq, dk, dv = pass_c(own_chunks + j, far_k(j, h))
            both = jnp.concatenate([dk, dv], axis=1)
            if part > 0:
                both = both + far_acc[j]
            if part < PARTS - 1:
                far_acc[j] = both
            else:
                gst[h, j] = both.astype(BF16)
            dq_acc[...] += dq
            return carry

        for o in range(own_chunks):
            dq, dk, dv = pass_c(o, own_kv(o, h)[0])
            at = slice(o * chunk, (o + 1) * chunk)
            both = jnp.concatenate([dk, dv], axis=1)
            own_acc[h, at, :] = both if part == 0 else own_acc[h, at, :] + both
            if o == 0:
                dq_acc[...] = dq
            else:
                dq_acc[...] += dq
        lax.fori_loop(0, me, far_c, 0)
        for gr in range(sub):
            done = (dq_acc[gr * rows : (gr + 1) * rows, :] * scale).astype(BF16)
            dq_ref[:, head_cols(u * sub + gr)] = done
            qall[u, alpha, :, head_cols(gr)] = done
        for mm in range(a):

            @pl.when(alpha != mm)
            def _():
                q_copy(u, mm).start()

        def send_g(j, carry):
            g_copy(h, me, j).start()
            return carry

        if part == PARTS - 1:
            lax.fori_loop(0, me, send_g, 0)

    def weight_part(h, wait_x):
        if wait_x:
            for m in range(a):
                for bb in range(b):
                    @pl.when(lax.div(bb * a + alpha, n_chunk) != t)
                    def _():
                        remote(
                            xst.at[0], xbuf.at[m, bb], x_send.at[0], x_recv.at[m, bb], me, t
                        ).wait_recv()

        for mm in range(a):

            @pl.when(alpha != mm)
            def _():
                remote(
                    qall.at[h, mm], qall.at[h, mm], q_send.at[h, mm], q_recv.at[h, mm], me, t
                ).wait_recv()

        def partial(bb):
            out = dot_tn(xbuf[0, bb], qall[h, 0])
            for m in range(1, a):
                out = out + dot_tn(xbuf[m, bb], qall[h, m])
            return out

        for d in range(1, b):
            bb = lax.rem(beta + d, b)
            wst[h, bb] = partial(bb).astype(BF16)
            w_copy(h, bb).start()
        w_own[h] = partial(beta)

    units = heads * PARTS
    for u in range(units):
        attend(u, u == 0)
    weight_part(units - 1, units == 1)

    for h in range(heads):

        def add_far(i, carry):
            remote(gst.at[h, 0], grecv.at[h, i], g_send.at[h, 0], g_recv.at[h, i], me, t).wait_recv()
            picks = slots(i, me)
            for p in range(local):
                got = grecv[h, i, p * KB : (p + 1) * KB, :].astype(F32)
                for blk in range(owner):
                    own_acc[h, blk * KB : (blk + 1) * KB, :] += jnp.where(
                        picks[p][blk] > 0, got, 0.0
                    )
            return carry

        lax.fori_loop(me + 1, n, add_far, 0)
        dk_ref[:, head_cols(h)] = own_acc[h, :, 0:HEAD_SIZE].astype(BF16)
        dv_ref[:, head_cols(h)] = own_acc[h, :, HEAD_SIZE : 2 * HEAD_SIZE].astype(BF16)

    for h in range(units):
        total = w_own[h]
        for d in range(1, b):
            bb = lax.rem(beta + d, b)
            remote(
                wst.at[h, bb], wrecv.at[h, bb], w_send.at[h, bb], w_recv.at[h, bb], me, t
            ).wait_recv()
            total = total + wrecv[h, bb].astype(F32)
        w_ref[:, h * gcols : (h + 1) * gcols] = total

    def done_kv(i, carry):
        kv_copy(i, me).wait_send()
        return carry

    lax.fori_loop(me + 1, n, done_kv, 0)
    for q in range(n_chunk):
        mine = lax.rem(t * n_chunk + q, a) == alpha

        @pl.when(jnp.logical_not(mine))
        def _():
            x_copy(q).wait_send()

        @pl.when(mine)
        def _():
            for m in range(a):
                for d in range(1, tp):
                    x_hand(q, m, d).wait_send()

    for h in range(heads):

        def done_g(j, carry):
            g_copy(h, me, j).wait_send()
            return carry

        lax.fori_loop(0, me, done_g, 0)
    for h in range(units):
        for mm in range(a):

            @pl.when(alpha != mm)
            def _():
                q_copy(h, mm).wait_send()

        for d in range(1, b):
            w_copy(h, lax.rem(beta + d, b)).wait_send()


def hand_out(*refs):
    for src, dst in zip(refs[:4], refs[4:]):
        dst[...] = src[...]


def body(n, tp, inputs, queries, key_vectors, value_rows_by_head, out_grad, chosen):
    rows, cols = key_vectors.shape
    q_cols = queries.shape[1]
    heads = cols // HEAD_SIZE
    group = q_cols // cols
    local = rows // QB
    chunk = local * KB
    own_chunks = rows // chunk
    sub = group // PARTS
    wide = sub * rows
    d_model = inputs.shape[1] * tp
    width = d_model // n
    n_chunk = inputs.shape[1] // width
    a = 4
    b = n // a
    gcols = sub * HEAD_SIZE
    blocks = n * rows // KB
    named = chosen[:, :, None] == jnp.arange(blocks, dtype=jnp.int32)[None, None, :]
    sel = jnp.sum(named.astype(jnp.int32), axis=1)
    vmem = pl.BlockSpec(memory_space=pltpu.VMEM)
    dma = pltpu.SemaphoreType.DMA
    shapes = (
        jax.ShapeDtypeStruct((rows, q_cols), BF16),
        jax.ShapeDtypeStruct((rows, cols), BF16),
        jax.ShapeDtypeStruct((rows, cols), BF16),
        jax.ShapeDtypeStruct((width, q_cols), F32),
    )
    grads = pl.pallas_call(
        functools.partial(kernel, n, tp, a, b),
        out_shape=shapes,
        in_specs=[pl.BlockSpec(memory_space=pltpu.SMEM)] + [vmem] * 5,
        out_specs=(vmem,) * 4,
        scratch_shapes=[
            pltpu.VMEM((n, chunk, 2 * cols), BF16),
            pltpu.VMEM((n, chunk, 2 * cols), BF16),
            pltpu.VMEM((n_chunk, rows, width), BF16),
            pltpu.VMEM((a, b, rows, width), BF16),
            pltpu.VMEM((wide, HEAD_SIZE), BF16),
            pltpu.VMEM((wide, HEAD_SIZE), BF16),
            pltpu.VMEM((own_chunks + n - 1, chunk, wide), F32),
            pltpu.VMEM((own_chunks + n - 1, chunk, wide), F32),
            pltpu.VMEM((wide, HEAD_SIZE), F32),
            pltpu.VMEM((n, chunk, 2 * HEAD_SIZE), F32),
            pltpu.VMEM((heads, n, chunk, 2 * HEAD_SIZE), BF16),
            pltpu.VMEM((heads, n, chunk, 2 * HEAD_SIZE), BF16),
            pltpu.VMEM((heads, rows, 2 * HEAD_SIZE), F32),
            pltpu.VMEM((heads * PARTS, a, rows, gcols), BF16),
            pltpu.VMEM((heads * PARTS, b, width, gcols), BF16),
            pltpu.VMEM((heads * PARTS, b, width, gcols), BF16),
            pltpu.VMEM((heads * PARTS, width, gcols), F32),
            dma((n,)),
            dma((n,)),
            dma((n_chunk,)),
            dma((n_chunk, a, tp - 1)),
            dma((a, b)),
            dma((heads, n)),
            dma((heads, n)),
            dma((heads * PARTS, a)),
            dma((heads * PARTS, a)),
            dma((heads * PARTS, b)),
            dma((heads * PARTS, b)),
        ],
        compiler_params=pltpu.CompilerParams(
            collective_id=0, has_side_effects=True, vmem_limit_bytes=60 * 1024 * 1024
        ),
    )(sel, inputs, queries, key_vectors, value_rows_by_head, out_grad)
    return pl.pallas_call(
        hand_out, out_shape=shapes, in_specs=[vmem] * 4, out_specs=(vmem,) * 4
    )(*grads)


def solution(mesh):
    n, tp = mesh.shape["kv"], mesh.shape["tp"]
    placed = (P("kv", "tp"),) * 5 + (P(),)
    return jax.shard_map(
        functools.partial(body, n, tp),
        mesh=mesh,
        in_specs=placed,
        out_specs=(P("kv", "tp"),) * 4,
        check_vma=False,
    )
```
